32 devices in a mesh: sp: 8 (over z, y), tp: 4 (over x, core).
Axes of the slice: x: 2, y: 2, z: 4, core: 2. Of those that a mesh axis runs over, the one named last changes fastest.
Arguments:
- moe_input: bfloat16 [1024, 2048], P('sp', 'tp'), may hold values from -6 to 6
- cotangent: bfloat16 [1024, 2048], P('sp', 'tp'), may hold values from -6 to 6
- expert_ids: int32 [1024, 2], P('sp'), may hold values from 0 to 7, as said below
- routing_weights: float32 [1024, 2], P('sp'), may hold values from 0.1 to 0.6
- gate_weight: bfloat16 [8, 2048, 1024], P('sp', None, 'tp'), may hold values from -0.125 to 0.125
- up_weight: bfloat16 [8, 2048, 1024], P('sp', None, 'tp'), may hold values from -0.125 to 0.125
- down_weight: bfloat16 [8, 1024, 2048], P('sp', 'tp'), may hold values from -0.1875 to 0.1875
- inner_x: bfloat16 [1024, 4096], P('sp', 'tp'), may hold values from -6 to 6
- inner_b: bfloat16 [1024, 256], P('sp', 'tp'), may hold values from -6 to 6
- inner_c: bfloat16 [1024, 256], P('sp', 'tp'), may hold values from -6 to 6
- gate_z: bfloat16 [1024, 4096], P('sp', 'tp'), may hold values from -6 to 6
- step_raw: float32 [1024, 64], P('sp', 'tp'), may hold values from -30 to 2
- decay_rate: float32 [64], P('tp'), may hold values from 1 to 16
- skip_weight: float32 [64], P('tp'), may hold values from 0.1 to 1.9
- norm_gain: float32 [4096], P('tp'), may hold values from 0.1 to 1.9
- w_out: bfloat16 [2048, 4096], P(None, 'tp'), may hold values from -0.09375 to 0.09375
Outputs:
- gate_weight_gradient: bfloat16 [8, 2048, 1024], P('sp', None, 'tp')
- up_weight_gradient: bfloat16 [8, 2048, 1024], P('sp', None, 'tp')
- down_weight_gradient: bfloat16 [8, 1024, 2048], P('sp', 'tp')
- grad_out: float32 [2048, 4096], P('sp', 'tp')
- grad_inner_x: bfloat16 [1024, 4096], P('sp', 'tp')
- grad_inner_b: float32 [1024, 256], P('sp', 'tp')
- grad_inner_c: float32 [1024, 256], P('sp', 'tp')
- grad_gate_z: bfloat16 [1024, 4096], P('sp', 'tp')
- grad_step_raw: float32 [1024, 64], P('sp', 'tp')
The draws below stay inside these ranges and needn't reach their ends.
Inputs may be any that keep to these rules, and one draw needn't show every extreme that they name: `expert_ids`: the two entries of a row differ and lie in the same group of 2 consecutive experts. In each aligned block of 128 rows no expert is named more than 64 times; one group of experts, the same for all blocks, takes exactly half of every block's rows, and each of its experts is named exactly 64 times in every block.
All inputs are finite; a program needn't handle non-finite values.
Results may differ from the reference program's by a relative error of at most 0.015.
Values may be sent and summed in bfloat16 or wider, within the bound.
A program may use at most 128 MiB of HBM per device.

```python
import math
from functools import partial
import jax
import jax.numpy as jnp
from jax import lax

D = 2048
HEADS = 64
HEAD_DIM = 64
GROUPS = 4
STATE = 64
SPAN = 128
FF = 1024
MOE_GROUPS = 4
TOP = 2
EXP_DEV = 1
TOKENS_PER_SHARD = 128
TOKENS = 1024
INNER = 4096
EXPERTS = 8
N_SP = 8
N_TP = 4


def head_laws(key):
    keys = jax.random.split(jax.random.fold_in(key, 101), 4)
    share = 0.5
    quick_head = jax.random.uniform(keys[0], (HEADS,), jnp.float32) < share
    decays = jnp.exp(jax.random.uniform(keys[1], (HEADS,), jnp.float32, 0.0, math.log(16.0)))
    quick = jnp.exp(jax.random.uniform(keys[2], (HEADS,), jnp.float32, math.log(1.0 / 120.0), math.log(1.0 / 40.0)))
    lasting = jnp.exp(jax.random.uniform(keys[3], (HEADS,), jnp.float32, math.log(0.1 / TOKENS), math.log(0.8 / TOKENS)))
    target = jnp.where(quick_head, quick, lasting)
    return (decays, target / decays)


def draw_decay_rate(key, part):
    return head_laws(key)[0]


def draw_step_raw(key, part):
    base_step = head_laws(key)[1]
    offsets = jnp.log(jnp.expm1(base_step))
    keys = jax.random.split(jax.random.fold_in(key, 202), 2)
    blocks = TOKENS // SPAN
    noise = jax.random.truncated_normal(keys[0], -2.5, 2.5, (TOKENS, HEADS), jnp.float32) * 0.7
    level = jax.random.uniform(keys[1], (blocks, 1, 1), jnp.float32, -0.7, 0.7)
    field = noise.reshape(blocks, SPAN, HEADS) + level
    return field.reshape(TOKENS, HEADS) + offsets[None, :]


def draw_expert_ids(key, part):
    expert_list = EXP_DEV * N_SP
    per_group = expert_list // MOE_GROUPS
    blocks = N_SP
    keys = jax.random.split(jax.random.fold_in(key, 303), 5)

    def shuffled(key_one):
        return jax.random.permutation(key_one, TOKENS_PER_SHARD)

    def mixed_table(key_one):
        return jax.random.permutation(key_one, per_group)
    full_group = jax.random.randint(keys[0], (), 0, MOE_GROUPS)
    order = jax.vmap(shuffled)(jax.random.split(keys[1], blocks))
    position = jnp.arange(TOKENS_PER_SHARD, dtype=jnp.int32)
    others = (full_group + 1 + jax.random.randint(keys[2], (blocks, TOKENS_PER_SHARD), 0, MOE_GROUPS - 1)) % MOE_GROUPS
    group_at = jnp.where(position[None, :] < TOKENS_PER_SHARD // 2, full_group, others).astype(jnp.int32)
    onehot = (group_at[:, :, None] == jnp.arange(MOE_GROUPS, dtype=jnp.int32)[None, None, :]).astype(jnp.int32)
    ranks = jnp.sum((jnp.cumsum(onehot, axis=1) - onehot) * onehot, axis=2)
    routing_tables = jax.vmap(mixed_table)(jax.random.split(keys[3], blocks * MOE_GROUPS)).reshape(blocks, MOE_GROUPS, per_group)
    offsets = jax.random.randint(keys[4], (blocks, MOE_GROUPS), 1, per_group)
    table_at = jnp.take_along_axis(routing_tables, jnp.broadcast_to(group_at[:, :, None], (blocks, TOKENS_PER_SHARD, per_group)), axis=1)
    shift_at = jnp.take_along_axis(offsets, group_at, axis=1)
    first = jnp.take_along_axis(table_at, (ranks % per_group)[:, :, None], axis=2)[:, :, 0]
    second = jnp.take_along_axis(table_at, ((ranks + shift_at) % per_group)[:, :, None], axis=2)[:, :, 0]
    chosen = jnp.stack([first, second], axis=2) + group_at[:, :, None] * per_group
    row_index = jnp.arange(blocks, dtype=jnp.int32)[:, None]
    placed = jnp.zeros((blocks, TOKENS_PER_SHARD, TOP), jnp.int32).at[row_index, order].set(chosen)
    return placed.reshape(blocks * TOKENS_PER_SHARD, TOP)


def strengthened(values, key, source, target, shards_of, factor):
    def block_of(dim):
        return (jnp.arange(values.shape[dim]) // (values.shape[dim] // shards_of)).reshape((-1,) + (1,) * (values.ndim - 1 - dim))

    near = jax.random.permutation(key, shards_of)[block_of(target)]
    second = (block_of(target) + shards_of // 2) % shards_of
    return jnp.where((block_of(source) == near) | (block_of(source) == second), factor * values, values)


def steps_of(stream_key, shape, pieces, smallest, top_value):
    gain, own = 1.0, jax.random.fold_in(stream_key, 6)
    for dim, blocks in pieces:
        draws = jnp.exp(jax.random.uniform(jax.random.fold_in(own, dim), (blocks,), jnp.float32, smallest / len(pieces), top_value / len(pieces)))
        gain = gain * jnp.repeat(draws, shape[dim] // blocks).reshape([-1 if axis == dim else 1 for axis in range(len(shape))])
    return gain


def gaussian(stream_key, dims, deviation, reach, cuts=(), held_as=jnp.bfloat16):
    array = deviation * jax.random.normal(stream_key, dims, jnp.float32)
    if cuts:
        array = array * steps_of(stream_key, dims, cuts, -0.22, 0.18)
    return jnp.clip(array, -reach, reach).astype(held_as)


def noise_with(key, dims, spread, reach, cuts, heavy, kind=jnp.bfloat16):
    array = spread * jax.random.normal(key, dims, jnp.float32)
    if cuts:
        array = array * steps_of(key, dims, cuts, -0.22, 0.18)
    return jnp.clip(strengthened(array, jax.random.fold_in(key, 3), *heavy), -reach, reach).astype(kind)


def setup_inputs(seed: int = 0) -> dict:
    streams_of = jax.random.split(jax.random.key(seed), 17)
    moe_input = gaussian(streams_of[0], (TOKENS, D), 1.0, 6.0, ((0, 8), (1, 4)))
    cotangent = noise_with(streams_of[1], (TOKENS, D), 1.0, 6.0, ((0, 8), (1, 4)), (0, 1, 8, 2.0))
    expert_ids = draw_expert_ids(jax.random.fold_in(streams_of[16], 71), 0)
    routing_weights = jnp.clip(0.1 + 0.5 * jax.random.uniform(streams_of[3], (TOKENS, TOP), jnp.float32) ** steps_of(streams_of[3], (TOKENS, TOP), ((0, 8),), -0.2, 0.2), 0.1, 0.6)
    gate_weight = gaussian(streams_of[4], (EXPERTS, D, FF), D ** -0.5, 0.125, ((0, 8), (2, 4)))
    up_weight = gaussian(streams_of[5], (EXPERTS, D, FF), D ** -0.5, 0.125, ((0, 8), (2, 4)))
    down_weight = gaussian(streams_of[6], (EXPERTS, FF, D), FF ** -0.5, 0.1875, ((0, 8), (1, 4)))
    inner_x = gaussian(streams_of[7], (TOKENS, INNER), 1.0, 6.0, ((0, 8), (1, 4)))
    inner_b = gaussian(streams_of[8], (TOKENS, GROUPS * STATE), 1.0, 6.0, ((0, 8), (1, 4)))
    inner_c = gaussian(streams_of[9], (TOKENS, GROUPS * STATE), 1.0, 6.0, ((0, 8), (1, 4)))
    gate_z = gaussian(streams_of[10], (TOKENS, INNER), 1.0, 6.0, ((0, 8), (1, 4)))
    step_raw = draw_step_raw(jax.random.fold_in(streams_of[16], 71), 0)
    decay_rate = draw_decay_rate(jax.random.fold_in(streams_of[16], 71), 0)
    skip_weight = jnp.clip(1.0 + 0.18 * jax.random.normal(streams_of[13], (HEADS,), jnp.float32), 0.1, 1.9)
    norm_gain = jnp.clip(1.0 + 0.18 * jax.random.normal(streams_of[14], (INNER,), jnp.float32), 0.1, 1.9)
    w_out = gaussian(streams_of[15], (D, INNER), INNER ** -0.5, 0.09375, ((1, 4),))
    return dict(moe_input=moe_input, cotangent=cotangent, expert_ids=expert_ids, routing_weights=routing_weights, gate_weight=gate_weight, up_weight=up_weight, down_weight=down_weight, inner_x=inner_x, inner_b=inner_b, inner_c=inner_c, gate_z=gate_z, step_raw=step_raw, decay_rate=decay_rate, skip_weight=skip_weight, norm_gain=norm_gain, w_out=w_out)


EPS = 0.01
HIGH = lax.Precision.HIGHEST

def slot_positions(chosen, expert_list, expert_capacity):
    listed = chosen.reshape(-1)
    onehot = (listed[:, None] == jnp.arange(expert_list, dtype=jnp.int32)[None, :]).astype(jnp.int32)
    before = jnp.cumsum(onehot, axis=0) - onehot
    return listed * expert_capacity + lax.optimization_barrier(jnp.sum(before * onehot, axis=1))

def prepare(inner_x32, inner_b32, step_raw, decays):
    tok_rows = inner_x32.shape[0]
    heads = decays.shape[0]
    groups = inner_b32.shape[1] // STATE
    per_group = heads // groups
    blocks = tok_rows // SPAN
    x_act = jax.nn.silu(inner_x32).reshape(tok_rows, heads, HEAD_DIM)
    b_blocks = jax.nn.silu(inner_b32).reshape(blocks, SPAN, groups, STATE)
    step_size = jax.nn.softplus(step_raw)
    decay_log = (-step_size * decays[None, :]).reshape(blocks, SPAN, groups, per_group)
    scaled = (x_act * step_size[:, :, None]).reshape(blocks, SPAN, groups, per_group, HEAD_DIM)
    return (x_act, b_blocks, decay_log, scaled)

def block_outputs(carry_state, block_in):
    x_block, log_block, b_block, c_block = block_in
    span_len = x_block.shape[0]
    running = jnp.cumsum(log_block, axis=0)
    places = jnp.arange(span_len)
    causal = (places[:, None] >= places[None, :])[:, :, None, None]
    between = running[:, None] - running[None, :]
    weights = jnp.where(causal, jnp.exp(jnp.where(causal, between, 0.0)), 0.0)
    scores = jnp.einsum('lgn,sgn->lsg', c_block, b_block, precision=HIGH)
    inside = jnp.einsum('lsg,lsge,sgep->lgep', scores, weights, x_block, precision=HIGH)
    carried = jnp.einsum('lgn,gepn,lge->lgep', c_block, carry_state, jnp.exp(running), precision=HIGH)
    to_end = jnp.exp(running[-1] - running)
    fresh_state = jnp.einsum('lgn,lge,lgep->gepn', b_block, to_end, x_block, precision=HIGH)
    return (carry_state * jnp.exp(running[-1])[:, :, None, None] + fresh_state, inside + carried)

def mixer_output(inner_x32, inner_b32, inner_c32, gate_z32, step_raw, carry_in, decays, skip_weight, norm_gain):
    tok_rows = inner_x32.shape[0]
    heads = decays.shape[0]
    groups = inner_b32.shape[1] // STATE
    x_act, b_blocks, decay_log, scaled = prepare(inner_x32, inner_b32, step_raw, decays)
    c_blocks = jax.nn.silu(inner_c32).reshape(tok_rows // SPAN, SPAN, groups, STATE)
    outputs = lax.scan(block_outputs, carry_in, (scaled, decay_log, b_blocks, c_blocks))[1]
    mixed_out = outputs.reshape(tok_rows, heads, HEAD_DIM) + x_act * skip_weight[None, :, None]
    gated_out = mixed_out.reshape(tok_rows, heads * HEAD_DIM) * jax.nn.silu(gate_z32)
    grouped = gated_out.reshape(tok_rows, groups, -1)
    normed = grouped * lax.rsqrt(lax.optimization_barrier(jnp.mean(grouped * grouped, axis=2, keepdims=True)) + EPS)
    return normed.reshape(tok_rows, -1) * norm_gain[None, :]

def expert_backward(padded_input, padded_gradient, item):
    owner, scaling, gate_w, up_w, down_w = item
    rows_in = padded_input[owner]
    rows_grad = (padded_gradient[owner].astype(jnp.float32) * scaling[:, None]).astype(jnp.bfloat16)
    gate_pre = jnp.dot(rows_in, gate_w, preferred_element_type=jnp.float32)
    up_pre = jnp.dot(rows_in, up_w, preferred_element_type=jnp.float32)
    sigmoid_gate = jax.nn.sigmoid(gate_pre)
    active = gate_pre * sigmoid_gate
    hidden = (active * up_pre).astype(jnp.bfloat16)
    hidden_grad = jnp.dot(rows_grad, down_w.T, preferred_element_type=jnp.float32)
    gate_grad = (hidden_grad * up_pre * sigmoid_gate * (1.0 + gate_pre * (1.0 - sigmoid_gate))).astype(jnp.bfloat16)
    up_grad = (hidden_grad * active).astype(jnp.bfloat16)
    down_part = jnp.dot(hidden.T, rows_grad, preferred_element_type=jnp.float32).astype(jnp.bfloat16)
    gate_part = jnp.dot(rows_in.T, gate_grad, preferred_element_type=jnp.float32).astype(jnp.bfloat16)
    up_part = jnp.dot(rows_in.T, up_grad, preferred_element_type=jnp.float32).astype(jnp.bfloat16)
    width = gate_w.shape[1] // N_TP
    summed = jnp.zeros(rows_in.shape, jnp.float32)
    for quarter in range(N_TP):
        low_col = quarter * width
        term = jnp.dot(gate_grad[:, low_col:low_col + width], gate_w[:, low_col:low_col + width].T, preferred_element_type=jnp.float32)
        term = term + jnp.dot(up_grad[:, low_col:low_col + width], up_w[:, low_col:low_col + width].T, preferred_element_type=jnp.float32)
        summed = summed + lax.optimization_barrier(term.astype(jnp.bfloat16)).astype(jnp.float32)
    return (gate_part, up_part, down_part, summed.astype(jnp.bfloat16))

def reference(moe_input, cotangent, expert_ids, routing_weights, gate_weight, up_weight, down_weight, inner_x, inner_b, inner_c, gate_z, step_raw, decay_rate, skip_weight, norm_gain, w_out):
    expert_list = gate_weight.shape[0]
    chosen_count = expert_ids.shape[1]
    expert_capacity = 4 * TOKENS_PER_SHARD // expert_list
    width = moe_input.shape[1]
    place_into_slots = jax.vmap(partial(slot_positions, expert_list=expert_list, expert_capacity=expert_capacity))(expert_ids.reshape(N_SP, TOKENS_PER_SHARD, chosen_count))
    local_owner = jnp.arange(TOKENS_PER_SHARD * chosen_count, dtype=jnp.int32) // chosen_count

    def routing_tables(spots, weights_block, block_index):
        owner = jnp.full((expert_list * expert_capacity,), TOKENS, jnp.int32).at[spots].set(local_owner + block_index * TOKENS_PER_SHARD)
        scaling = jnp.zeros((expert_list * expert_capacity,), jnp.float32).at[spots].set(weights_block)
        return (owner, scaling)
    owning_experts, scale_factors = jax.vmap(routing_tables)(place_into_slots, routing_weights.reshape(N_SP, TOKENS_PER_SHARD * chosen_count), jnp.arange(N_SP, dtype=jnp.int32))
    owning_experts = owning_experts.reshape(N_SP, expert_list, expert_capacity).transpose(1, 0, 2).reshape(expert_list, N_SP * expert_capacity)
    scale_factors = scale_factors.reshape(N_SP, expert_list, expert_capacity).transpose(1, 0, 2).reshape(expert_list, N_SP * expert_capacity)
    padded_input = jnp.concatenate([moe_input, jnp.zeros((1, width), jnp.bfloat16)], axis=0)
    padded_gradient = jnp.concatenate([cotangent, jnp.zeros((1, width), jnp.bfloat16)], axis=0)
    gate_weight_gradient, up_weight_gradient, down_weight_gradient, slot_gradient = lax.map(partial(expert_backward, padded_input, padded_gradient), (owning_experts, scale_factors, gate_weight, up_weight, down_weight))
    by_block = slot_gradient.reshape(expert_list, N_SP, expert_capacity, width).transpose(1, 0, 2, 3).reshape(N_SP, expert_list * expert_capacity, width)

    def collect(rows_block, spots):
        return rows_block[spots].astype(jnp.float32)
    moe_grad = lax.optimization_barrier(jnp.sum(jax.vmap(collect)(by_block, place_into_slots).reshape(TOKENS, chosen_count, width), axis=1))
    mixer_grad = (cotangent.astype(jnp.float32) + moe_grad).astype(jnp.bfloat16)
    groups = inner_b.shape[1] // STATE
    per_group = decay_rate.shape[0] // groups
    zero_state = jnp.zeros((groups, per_group, HEAD_DIM, STATE), jnp.float32)

    def forward(x_in, b_in, c_in, z_in, raw_in):
        return mixer_output(x_in, b_in, c_in, z_in, raw_in, zero_state, decay_rate, skip_weight, norm_gain)
    normed, pullback = jax.vjp(forward, inner_x.astype(jnp.float32), inner_b.astype(jnp.float32), inner_c.astype(jnp.float32), gate_z.astype(jnp.float32), step_raw)
    norm_out = normed.astype(jnp.bfloat16)
    grad_out = jnp.dot(mixer_grad.T, norm_out, preferred_element_type=jnp.float32)
    norm_grad = jnp.dot(mixer_grad, w_out, preferred_element_type=jnp.float32)
    x_grad, b_grad, c_grad, z_grad, raw_grad = pullback(norm_grad)
    return (gate_weight_gradient, up_weight_gradient, down_weight_gradient, grad_out, x_grad.astype(jnp.bfloat16), b_grad, c_grad, z_grad.astype(jnp.bfloat16), raw_grad)
```

```python
from functools import partial

import jax
import jax.numpy as jnp
from jax import lax
from jax.experimental import pallas as pl
from jax.experimental.pallas import tpu as pltpu
from jax.sharding import PartitionSpec as P

HEAD_DIM = 64
STATE = 64
PAIR = 2 * HEAD_DIM
EPS = 0.01
HIGH = lax.Precision.HIGHEST
F32 = jnp.float32
BF16 = jnp.bfloat16


def call(kernel, outs, flops, scratch=()):
    return pl.pallas_call(
        kernel,
        out_shape=[jax.ShapeDtypeStruct(s, d) for s, d in outs],
        scratch_shapes=list(scratch),
        cost_estimate=pl.CostEstimate(flops=flops, bytes_accessed=4_000_000, transcendentals=0),
        compiler_params=pltpu.CompilerParams(vmem_limit_bytes=48 * 1024 * 1024),
    )


def nn(a, b):
    return jnp.dot(a.astype(BF16), b.astype(BF16), preferred_element_type=F32)


def tn(a, b):
    return lax.dot_general(
        a.astype(BF16), b.astype(BF16), (((0,), (0,)), ((), ())), preferred_element_type=F32
    )


def nt(a, b):
    return lax.dot_general(
        a.astype(BF16), b.astype(BF16), (((1,), (1,)), ((), ())), preferred_element_type=F32
    )


def spread(heads):
    rows = lax.broadcasted_iota(jnp.int32, (heads, heads * HEAD_DIM), 0)
    cols = lax.broadcasted_iota(jnp.int32, (heads, heads * HEAD_DIM), 1)
    return (cols // HEAD_DIM == rows).astype(F32)


def wide(v, table):
    return jnp.dot(v, table, precision=HIGH, preferred_element_type=F32)


def narrow(v, table):
    return lax.dot_general(
        v, table, (((1,), (1,)), ((), ())), precision=HIGH, preferred_element_type=F32
    )


def silu_and_slope(v):
    s = jax.nn.sigmoid(v)
    return v * s, s * (1.0 + v * (1.0 - s))


def silu(v):
    return v * jax.nn.sigmoid(v)


def causal_of(rows):
    return lax.broadcasted_iota(jnp.int32, (rows, rows), 0) >= lax.broadcasted_iota(
        jnp.int32, (rows, rows), 1
    )


def decay_table(causal, run_ref, run_t_ref, head):
    gap = run_ref[:, head : head + 1] - run_t_ref[head : head + 1, :]
    return jnp.where(causal, jnp.exp(jnp.where(causal, gap, 0.0)), 0.0)


def fresh_kernel(x_ref, b_ref, dt_ref, run_ref, fresh_ref):
    table = spread(dt_ref.shape[1])
    run = run_ref[...]
    factor = dt_ref[...] * jnp.exp(run[-1:, :] - run)
    xe = silu(x_ref[...].astype(F32)) * wide(factor, table)
    fresh_ref[...] = tn(silu(b_ref[...].astype(F32)), xe).astype(BF16)


def weighted_sum(all_ref, weight_ref):
    def one(j, total):
        return total + all_ref[j].astype(F32) * weight_ref[pl.ds(j, 1), :]

    return lax.fori_loop(0, all_ref.shape[0], one, jnp.zeros(all_ref.shape[1:], F32))


def forward_kernel(
    x_ref, b_ref, c_ref, z_ref, dt_ref, run_ref, run_t_ref, skip_ref, gain_ref, all_ref, coef_ref,
    norm_ref, mixed_ref, state_ref, weight_ref,
):
    heads = dt_ref.shape[1]
    table = spread(heads)
    weight_ref[...] = wide(coef_ref[...], table)
    state = weighted_sum(all_ref, weight_ref)
    state_ref[...] = state
    x_act = silu(x_ref[...].astype(F32))
    xs = (x_act * wide(dt_ref[...], table)).astype(BF16)
    b_act = silu(b_ref[...].astype(F32))
    c_act = silu(c_ref[...].astype(F32))
    mixed_ref[...] = nn(c_act, state) * wide(jnp.exp(run_ref[...]), table) + x_act * wide(
        skip_ref[...], table
    )
    rows = x_ref.shape[0]
    causal = causal_of(rows)
    scores = nt(c_act, b_act)
    first = lax.broadcasted_iota(jnp.int32, (rows, PAIR), 1) < HEAD_DIM
    for pair in range(heads // 2):
        lo = pair * PAIR
        part = xs[:, lo : lo + PAIR]
        one = nn(scores * decay_table(causal, run_ref, run_t_ref, 2 * pair), part)
        two = nn(scores * decay_table(causal, run_ref, run_t_ref, 2 * pair + 1), part)
        mixed_ref[:, lo : lo + PAIR] += jnp.where(first, one, two)
    gated = mixed_ref[...] * silu(z_ref[...].astype(F32))
    scale = lax.rsqrt(jnp.mean(gated * gated, axis=1, keepdims=True) + EPS)
    norm_ref[...] = (gated * scale * gain_ref[...]).astype(BF16)


def backward_kernel(
    x_ref, b_ref, c_ref, z_ref, dt_ref, run_ref, run_t_ref, skip_ref, gain_ref, mixed_ref,
    state_ref, up_ref,
    state_grad_ref, xs_grad_ref, x_grad_ref, z_grad_ref, run_grad_ref, b_grad_ref, c_grad_ref,
):
    heads = dt_ref.shape[1]
    rows = x_ref.shape[0]
    table = spread(heads)
    z_act, z_slope = silu_and_slope(z_ref[...].astype(F32))
    mixed = mixed_ref[...]
    gated = mixed * z_act
    scale = lax.rsqrt(jnp.mean(gated * gated, axis=1, keepdims=True) + EPS)
    up = up_ref[...] * gain_ref[...]
    inner = jnp.mean(up * gated, axis=1, keepdims=True)
    gated_grad = scale * (up - gated * (scale * scale * inner))
    z_grad_ref[...] = (gated_grad * mixed * z_slope).astype(BF16)
    dy = gated_grad * z_act
    x_act = silu(x_ref[...].astype(F32))
    x_grad_ref[...] = dy * wide(skip_ref[...], table)
    xs = (x_act * wide(dt_ref[...], table)).astype(BF16)
    b_act = silu(b_ref[...].astype(F32))
    c_act, c_slope = silu_and_slope(c_ref[...].astype(F32))
    state = state_ref[...]
    grown = dy * wide(jnp.exp(run_ref[...]), table)
    state_grad_ref[...] = tn(c_act, grown).astype(BF16)
    c_grad = nt(grown, state)
    run_grad = narrow(grown * nn(c_act, state), table)
    causal = causal_of(rows)
    scores = nt(c_act, b_act)
    scores_grad = jnp.zeros((rows, rows), F32)
    first = lax.broadcasted_iota(jnp.int32, (rows, PAIR), 1) < HEAD_DIM
    lane = lax.broadcasted_iota(jnp.int32, (rows, heads), 1)
    for pair in range(heads // 2):
        lo = pair * PAIR
        part = xs[:, lo : lo + PAIR]
        dy_part = dy[:, lo : lo + PAIR]
        got = []
        for k in range(2):
            head = 2 * pair + k
            decay = decay_table(causal, run_ref, run_t_ref, head)
            weights = scores * decay
            mine = jnp.where(first if k == 0 else ~first, dy_part, 0.0)
            got.append(tn(weights, mine))
            weights_grad = nt(mine, part)
            scores_grad += weights_grad * decay
            flow = weights_grad * weights
            change = jnp.sum(flow - flow.T, axis=1, keepdims=True)
            run_grad += jnp.where(lane == head, change, 0.0)
        xs_grad_ref[:, lo : lo + PAIR] = got[0] + got[1]
    run_grad_ref[...] = run_grad
    b_grad_ref[...] = tn(scores_grad, c_act)
    c_grad_ref[...] = (c_grad + nn(scores_grad, b_act)) * c_slope


def finish_kernel(
    x_ref, b_ref, raw_ref, dt_ref, run_ref, rate_ref, state_ref, all_ref, coef_ref, xs_grad_ref,
    x_grad_ref, run_grad_ref, b_grad_ref,
    x_out_ref, b_out_ref, raw_out_ref, weight_ref,
):
    heads = dt_ref.shape[1]
    rows = x_ref.shape[0]
    table = spread(heads)
    weight_ref[...] = wide(coef_ref[...], table)
    after = weighted_sum(all_ref, weight_ref)
    x_act, x_slope = silu_and_slope(x_ref[...].astype(F32))
    b_act, b_slope = silu_and_slope(b_ref[...].astype(F32))
    dt = dt_ref[...]
    dt_wide = wide(dt, table)
    run = run_ref[...]
    last = run[-1:, :]
    to_end = wide(jnp.exp(last - run), table)
    moved = nn(b_act, after) * to_end
    xs = x_act * dt_wide
    xs_grad = xs_grad_ref[...] + moved
    b_grad = b_grad_ref[...] + nt(xs * to_end, after)
    out_flow = narrow(xs * moved, table)
    whole = jnp.exp(last) * narrow(
        jnp.sum(after * state_ref[...], axis=0, keepdims=True), table
    )
    at_end = jnp.sum(out_flow, axis=0, keepdims=True) + whole
    run_grad = run_grad_ref[...] - out_flow
    causal = causal_of(rows).astype(F32)
    log_grad = at_end + lax.dot_general(
        causal, run_grad, (((0,), (0,)), ((), ())), precision=HIGH, preferred_element_type=F32
    )
    dt_grad = narrow(x_act * xs_grad, table) - rate_ref[...] * log_grad
    raw_out_ref[...] = dt_grad * jax.nn.sigmoid(raw_ref[...])
    b_out_ref[...] = b_grad * b_slope
    x_out_ref[...] = ((x_grad_ref[...] + xs_grad * dt_wide) * x_slope).astype(BF16)


def picks(ids, slots, experts):
    rows = ids.shape[0]
    capacity = slots // experts
    choice = lax.broadcasted_iota(jnp.int32, (rows, experts), 1)
    hot = [(ids[:, k : k + 1] == choice).astype(F32) for k in range(ids.shape[1])]
    strict = (
        lax.broadcasted_iota(jnp.int32, (rows, rows), 0)
        > lax.broadcasted_iota(jnp.int32, (rows, rows), 1)
    ).astype(F32)
    before = nn(strict, sum(hot))
    place = lax.broadcasted_iota(jnp.int32, (rows, slots), 1)
    found = []
    for k, one in enumerate(hot):
        rank = jnp.sum(before * one, axis=1, keepdims=True).astype(jnp.int32)
        found.append((place == ids[:, k : k + 1] * capacity + rank).astype(BF16))
    return found


def dispatch_kernel(experts, x_ref, cot_ref, ids_ref, weight_ref, out_ref):
    slots = out_ref.shape[0]
    cols = x_ref.shape[1]
    found = picks(ids_ref[...], slots, experts)
    cot = cot_ref[...].astype(F32)
    total = jnp.zeros((slots, cols), F32)
    for k, one in enumerate(found):
        total += tn(one, (cot * weight_ref[:, k : k + 1]).astype(BF16))
    out_ref[:, :cols] = tn(sum(found), x_ref[...]).astype(BF16)
    out_ref[:, cols:] = total.astype(BF16)


def combine_kernel(experts, back_ref, cot_ref, ids_ref, out_ref):
    found = picks(ids_ref[...], back_ref.shape[0], experts)
    moe_grad = nn(sum(found), back_ref[...])
    out_ref[...] = (cot_ref[...].astype(F32) + moe_grad).astype(BF16)


def carries(last, axis):
    count, me = lax.axis_size(axis), lax.axis_index(axis)
    ends = lax.all_gather(last, axis)
    j = jnp.arange(count)
    i = j[None, :]
    ahead = ((i > j[:, None]) & (i < me)).astype(F32)
    behind = ((i < j[:, None]) & (i > me)).astype(F32)
    fore = jnp.where((j < me)[:, None], jnp.exp(jnp.dot(ahead, ends, precision=HIGH)), 0.0)
    back = jnp.where((j > me)[:, None], jnp.exp(jnp.dot(behind, ends, precision=HIGH)), 0.0)
    return fore, back


def body(
    moe_input, cotangent, expert_ids, routing_weights, gate_weight, up_weight, down_weight,
    inner_x, inner_b, inner_c, gate_z, step_raw, decay_rate, skip_weight, norm_gain, w_out,
):
    rows, chosen = expert_ids.shape
    senders = lax.axis_size("sp")
    experts = gate_weight.shape[0] * senders
    capacity = 4 * rows // experts
    slots = experts * capacity
    cols = moe_input.shape[1]
    heads = decay_rate.shape[0]
    inner = heads * HEAD_DIM
    rate, skip, gain = decay_rate[None, :], skip_weight[None, :], norm_gain[None, :]

    dt = jax.nn.softplus(step_raw)
    run = jnp.cumsum(-dt * rate, axis=0)
    run_t = run.T
    (fresh,) = call(fresh_kernel, [((STATE, inner), BF16)], 40_000_000)(inner_x, inner_b, dt, run)
    fresh_all = lax.all_gather(fresh, "sp")
    fore, back = carries(run[-1], "sp")

    (sent,) = call(partial(dispatch_kernel, experts), [((slots, 2 * cols), BF16)], 200_000_000)(
        moe_input, cotangent, expert_ids, routing_weights
    )
    routed = lax.all_to_all(
        sent.reshape(senders, slots // senders, 2 * cols), "sp", 0, 0, tiled=True
    ).reshape(slots, 2 * cols)
    routed = lax.all_gather(routed, "tp")

    weight_rows = pltpu.VMEM((senders, inner), F32)
    norm_rows, mixed, state = call(
        forward_kernel,
        [((rows, inner), BF16), ((rows, inner), F32), ((STATE, inner), F32)],
        300_000_000,
        [weight_rows],
    )(inner_x, inner_b, inner_c, gate_z, dt, run, run_t, skip, gain, fresh_all, fore)
    norm_all = lax.all_gather(norm_rows, "sp", axis=0, tiled=True)

    routed_in = jnp.concatenate([routed[k, :, :cols] for k in range(routed.shape[0])], axis=1)
    routed_grad = jnp.concatenate([routed[k, :, cols:] for k in range(routed.shape[0])], axis=1)
    gate_w, up_w, down_w = gate_weight[0], up_weight[0], down_weight[0]
    gate_pre = jnp.dot(routed_in, gate_w, preferred_element_type=F32)
    up_pre = jnp.dot(routed_in, up_w, preferred_element_type=F32)
    sig = jax.nn.sigmoid(gate_pre)
    active = gate_pre * sig
    hidden = (active * up_pre).astype(BF16)
    hidden_grad = nt(routed_grad, down_w)
    gate_grad = (hidden_grad * up_pre * sig * (1.0 + gate_pre * (1.0 - sig))).astype(BF16)
    up_grad = (hidden_grad * active).astype(BF16)
    terms = (nt(gate_grad, gate_w) + nt(up_grad, up_w)).astype(BF16)
    summed = lax.psum_scatter(terms, "tp", scatter_dimension=1, tiled=True)
    returned = lax.all_to_all(
        summed.reshape(senders, slots // senders, cols), "sp", 0, 0, tiled=True
    ).reshape(slots, cols)
    (mixer_cols,) = call(partial(combine_kernel, experts), [((rows, cols), BF16)], 100_000_000)(
        returned, cotangent, expert_ids
    )
    mixer_rows = lax.all_gather(mixer_cols, "tp", axis=1, tiled=True)
    norm_grad = jnp.dot(mixer_rows, w_out, preferred_element_type=F32)
    state_grad, xs_grad, x_grad, z_grad, run_grad, b_grad, c_grad = call(
        backward_kernel,
        [
            ((STATE, inner), BF16),
            ((rows, inner), F32),
            ((rows, inner), F32),
            ((rows, inner), BF16),
            ((rows, heads), F32),
            ((rows, STATE), F32),
            ((rows, STATE), F32),
        ],
        600_000_000,
    )(inner_x, inner_b, inner_c, gate_z, dt, run, run_t, skip, gain, mixed, state, norm_grad)
    state_grads = lax.all_gather(state_grad, "sp")
    depth = mixer_rows.shape[1] // senders
    mixer_blocks = jnp.swapaxes(mixer_rows.reshape(rows, senders, depth), 0, 1)
    mixer_all = lax.all_to_all(mixer_blocks, "sp", 0, 0, tiled=True).reshape(rows * senders, depth)
    grad_out = tn(mixer_all, norm_all)
    gate_weight_gradient = tn(routed_in, gate_grad).astype(BF16)[None]
    up_weight_gradient = tn(routed_in, up_grad).astype(BF16)[None]
    down_weight_gradient = tn(hidden, routed_grad).astype(BF16)[None]
    grad_inner_x, grad_inner_b, grad_step_raw = call(
        finish_kernel,
        [((rows, inner), BF16), ((rows, STATE), F32), ((rows, heads), F32)],
        300_000_000,
        [weight_rows],
    )(
        inner_x, inner_b, step_raw, dt, run, rate, state, state_grads, back, xs_grad, x_grad,
        run_grad, b_grad,
    )
    return (
        gate_weight_gradient, up_weight_gradient, down_weight_gradient, grad_out, grad_inner_x,
        grad_inner_b, c_grad, z_grad, grad_step_raw,
    )


def solution(mesh):
    row = P("sp", "tp")
    deep, flat, tall = P("sp", None, "tp"), P("sp", None), P("sp", "tp", None)
    return jax.shard_map(
        body,
        mesh=mesh,
        in_specs=(
            row, row, flat, flat, deep, deep, tall, row, row, row, row, row,
            P("tp"), P("tp"), P("tp"), P(None, "tp"),
        ),
        out_specs=(deep, deep, tall, row, row, row, row, row, row),
        check_vma=False,
    )
```

```python
from functools import partial

import jax
import jax.numpy as jnp
from jax import lax
from jax.experimental import pallas as pl
from jax.experimental.pallas import tpu as pltpu
from jax.sharding import PartitionSpec as P

HEAD_DIM = 64
STATE = 64
PAIR = 2 * HEAD_DIM
EPS = 0.01
HIGH = lax.Precision.HIGHEST
F32 = jnp.float32
BF16 = jnp.bfloat16


def call(kernel, outs, flops, scratch=()):
    return pl.pallas_call(
        kernel,
        out_shape=[jax.ShapeDtypeStruct(s, d) for s, d in outs],
        scratch_shapes=list(scratch),
        cost_estimate=pl.CostEstimate(flops=flops, bytes_accessed=4_000_000, transcendentals=0),
        compiler_params=pltpu.CompilerParams(vmem_limit_bytes=48 * 1024 * 1024),
    )


def nn(a, b):
    return jnp.dot(a.astype(BF16), b.astype(BF16), preferred_element_type=F32)


def tn(a, b):
    return lax.dot_general(
        a.astype(BF16), b.astype(BF16), (((0,), (0,)), ((), ())), preferred_element_type=F32
    )


def nt(a, b):
    return lax.dot_general(
        a.astype(BF16), b.astype(BF16), (((1,), (1,)), ((), ())), preferred_element_type=F32
    )


def spread(heads):
    rows = lax.broadcasted_iota(jnp.int32, (heads, heads * HEAD_DIM), 0)
    cols = lax.broadcasted_iota(jnp.int32, (heads, heads * HEAD_DIM), 1)
    return (cols // HEAD_DIM == rows).astype(F32)


def wide(v, table):
    return jnp.dot(v, table, precision=HIGH, preferred_element_type=F32)


def narrow(v, table):
    return lax.dot_general(
        v, table, (((1,), (1,)), ((), ())), precision=HIGH, preferred_element_type=F32
    )


def silu_and_slope(v):
    s = jax.nn.sigmoid(v)
    return v * s, s * (1.0 + v * (1.0 - s))


def silu(v):
    return v * jax.nn.sigmoid(v)


def causal_of(rows):
    return lax.broadcasted_iota(jnp.int32, (rows, rows), 0) >= lax.broadcasted_iota(
        jnp.int32, (rows, rows), 1
    )


def decay_table(causal, run_ref, run_t_ref, head):
    gap = run_ref[:, head : head + 1] - run_t_ref[head : head + 1, :]
    return jnp.where(causal, jnp.exp(jnp.where(causal, gap, 0.0)), 0.0)


def fresh_kernel(x_ref, b_ref, dt_ref, run_ref, fresh_ref):
    table = spread(dt_ref.shape[1])
    run = run_ref[...]
    factor = dt_ref[...] * jnp.exp(run[-1:, :] - run)
    xe = silu(x_ref[...].astype(F32)) * wide(factor, table)
    fresh_ref[...] = tn(silu(b_ref[...].astype(F32)), xe).astype(BF16)


def weighted_sum(all_ref, weight_ref):
    def one(j, total):
        return total + all_ref[j].astype(F32) * weight_ref[pl.ds(j, 1), :]

    return lax.fori_loop(0, all_ref.shape[0], one, jnp.zeros(all_ref.shape[1:], F32))


def forward_kernel(
    x_ref, b_ref, c_ref, z_ref, dt_ref, run_ref, run_t_ref, skip_ref, gain_ref, all_ref, coef_ref,
    norm_ref, mixed_ref, state_ref, weight_ref,
):
    heads = dt_ref.shape[1]
    table = spread(heads)
    weight_ref[...] = wide(coef_ref[...], table)
    state = weighted_sum(all_ref, weight_ref)
    state_ref[...] = state
    x_act = silu(x_ref[...].astype(F32))
    xs = (x_act * wide(dt_ref[...], table)).astype(BF16)
    b_act = silu(b_ref[...].astype(F32))
    c_act = silu(c_ref[...].astype(F32))
    mixed_ref[...] = nn(c_act, state) * wide(jnp.exp(run_ref[...]), table) + x_act * wide(
        skip_ref[...], table
    )
    rows = x_ref.shape[0]
    causal = causal_of(rows)
    scores = nt(c_act, b_act)
    first = lax.broadcasted_iota(jnp.int32, (rows, PAIR), 1) < HEAD_DIM
    for pair in range(heads // 2):
        lo = pair * PAIR
        part = xs[:, lo : lo + PAIR]
        one = nn(scores * decay_table(causal, run_ref, run_t_ref, 2 * pair), part)
        two = nn(scores * decay_table(causal, run_ref, run_t_ref, 2 * pair + 1), part)
        mixed_ref[:, lo : lo + PAIR] += jnp.where(first, one, two)
    gated = mixed_ref[...] * silu(z_ref[...].astype(F32))
    scale = lax.rsqrt(jnp.mean(gated * gated, axis=1, keepdims=True) + EPS)
    norm_ref[...] = (gated * scale * gain_ref[...]).astype(BF16)


def backward_kernel(
    x_ref, b_ref, c_ref, z_ref, dt_ref, run_ref, run_t_ref, skip_ref, gain_ref, mixed_ref,
    state_ref, up_ref,
    state_grad_ref, xs_grad_ref, x_grad_ref, z_grad_ref, run_grad_ref, b_grad_ref, c_grad_ref,
):
    heads = dt_ref.shape[1]
    rows = x_ref.shape[0]
    table = spread(heads)
    z_act, z_slope = silu_and_slope(z_ref[...].astype(F32))
    mixed = mixed_ref[...]
    gated = mixed * z_act
    scale = lax.rsqrt(jnp.mean(gated * gated, axis=1, keepdims=True) + EPS)
    up = up_ref[...] * gain_ref[...]
    inner = jnp.mean(up * gated, axis=1, keepdims=True)
    gated_grad = scale * (up - gated * (scale * scale * inner))
    z_grad_ref[...] = (gated_grad * mixed * z_slope).astype(BF16)
    dy = gated_grad * z_act
    x_act = silu(x_ref[...].astype(F32))
    x_grad_ref[...] = dy * wide(skip_ref[...], table)
    xs = (x_act * wide(dt_ref[...], table)).astype(BF16)
    b_act = silu(b_ref[...].astype(F32))
    c_act, c_slope = silu_and_slope(c_ref[...].astype(F32))
    state = state_ref[...]
    grown = dy * wide(jnp.exp(run_ref[...]), table)
    state_grad_ref[...] = tn(c_act, grown).astype(BF16)
    c_grad = nt(grown, state)
    run_grad = narrow(grown * nn(c_act, state), table)
    causal = causal_of(rows)
    scores = nt(c_act, b_act)
    scores_grad = jnp.zeros((rows, rows), F32)
    first = lax.broadcasted_iota(jnp.int32, (rows, PAIR), 1) < HEAD_DIM
    lane = lax.broadcasted_iota(jnp.int32, (rows, heads), 1)
    for pair in range(heads // 2):
        lo = pair * PAIR
        part = xs[:, lo : lo + PAIR]
        dy_part = dy[:, lo : lo + PAIR]
        got = []
        for k in range(2):
            head = 2 * pair + k
            decay = decay_table(causal, run_ref, run_t_ref, head)
            weights = scores * decay
            mine = jnp.where(first if k == 0 else ~first, dy_part, 0.0)
            got.append(tn(weights, mine))
            weights_grad = nt(mine, part)
            scores_grad += weights_grad * decay
            flow = weights_grad * weights
            change = jnp.sum(flow - flow.T, axis=1, keepdims=True)
            run_grad += jnp.where(lane == head, change, 0.0)
        xs_grad_ref[:, lo : lo + PAIR] = got[0] + got[1]
    run_grad_ref[...] = run_grad
    b_grad_ref[...] = tn(scores_grad, c_act)
    c_grad_ref[...] = (c_grad + nn(scores_grad, b_act)) * c_slope


def finish_kernel(
    x_ref, b_ref, raw_ref, dt_ref, run_ref, rate_ref, state_ref, all_ref, coef_ref, xs_grad_ref,
    x_grad_ref, run_grad_ref, b_grad_ref,
    x_out_ref, b_out_ref, raw_out_ref, weight_ref,
):
    heads = dt_ref.shape[1]
    rows = x_ref.shape[0]
    table = spread(heads)
    weight_ref[...] = wide(coef_ref[...], table)
    after = weighted_sum(all_ref, weight_ref)
    x_act, x_slope = silu_and_slope(x_ref[...].astype(F32))
    b_act, b_slope = silu_and_slope(b_ref[...].astype(F32))
    dt = dt_ref[...]
    dt_wide = wide(dt, table)
    run = run_ref[...]
    last = run[-1:, :]
    to_end = wide(jnp.exp(last - run), table)
    moved = nn(b_act, after) * to_end
    xs = x_act * dt_wide
    xs_grad = xs_grad_ref[...] + moved
    b_grad = b_grad_ref[...] + nt(xs * to_end, after)
    out_flow = narrow(xs * moved, table)
    whole = jnp.exp(last) * narrow(
        jnp.sum(after * state_ref[...], axis=0, keepdims=True), table
    )
    at_end = jnp.sum(out_flow, axis=0, keepdims=True) + whole
    run_grad = run_grad_ref[...] - out_flow
    causal = causal_of(rows).astype(F32)
    log_grad = at_end + lax.dot_general(
        causal, run_grad, (((0,), (0,)), ((), ())), precision=HIGH, preferred_element_type=F32
    )
    dt_grad = narrow(x_act * xs_grad, table) - rate_ref[...] * log_grad
    raw_out_ref[...] = dt_grad * jax.nn.sigmoid(raw_ref[...])
    b_out_ref[...] = b_grad * b_slope
    x_out_ref[...] = ((x_grad_ref[...] + xs_grad * dt_wide) * x_slope).astype(BF16)


def picks(ids, slots, experts):
    rows = ids.shape[0]
    capacity = slots // experts
    choice = lax.broadcasted_iota(jnp.int32, (rows, experts), 1)
    hot = [(ids[:, k : k + 1] == choice).astype(F32) for k in range(ids.shape[1])]
    strict = (
        lax.broadcasted_iota(jnp.int32, (rows, rows), 0)
        > lax.broadcasted_iota(jnp.int32, (rows, rows), 1)
    ).astype(F32)
    before = nn(strict, sum(hot))
    place = lax.broadcasted_iota(jnp.int32, (rows, slots), 1)
    found = []
    for k, one in enumerate(hot):
        rank = jnp.sum(before * one, axis=1, keepdims=True).astype(jnp.int32)
        found.append((place == ids[:, k : k + 1] * capacity + rank).astype(BF16))
    return found


def dispatch_kernel(experts, x_ref, cot_ref, ids_ref, weight_ref, out_ref):
    slots = out_ref.shape[1]
    cols = x_ref.shape[1]
    found = picks(ids_ref[...], slots, experts)
    cot = cot_ref[...].astype(F32)
    total = jnp.zeros((slots, cols), F32)
    for k, one in enumerate(found):
        total += tn(one, (cot * weight_ref[:, k : k + 1]).astype(BF16))
    out_ref[0] = tn(sum(found), x_ref[...]).astype(BF16)
    out_ref[1] = total.astype(BF16)


def combine_kernel(experts, back_ref, cot_ref, ids_ref, out_ref):
    found = picks(ids_ref[...], back_ref.shape[0], experts)
    moe_grad = nn(sum(found), back_ref[...])
    out_ref[...] = (cot_ref[...].astype(F32) + moe_grad).astype(BF16)


MESH = pl.DeviceIdType.MESH


def greet(count, me, others):
    barrier = pltpu.get_barrier_semaphore()

    def one(d, _):
        pl.semaphore_signal(
            barrier, inc=1, device_id={"sp": lax.rem(me + d, count)}, device_id_type=MESH
        )
        return 0

    lax.fori_loop(1, count, one, 0)
    for other in others:
        pl.semaphore_signal(barrier, inc=1, device_id={"tp": other}, device_id_type=MESH)
    pl.semaphore_wait(barrier, count - 1 + len(others))


def partners():
    t = lax.axis_index("tp")
    half = lax.axis_size("tp") // 2
    far = lax.rem(t + half, 2 * half)
    near = t + 1 - 2 * lax.rem(t, 2)
    return t, far, near


def route_kernel(
    count, sent_ref, out_ref, own_sem, sp_send, sp_recv, far_send, far_recv, near_send, near_recv
):
    cols = sent_ref.shape[3]
    me = lax.axis_index("sp")
    t, far, near = partners()

    def at(block, place):
        return out_ref.at[:, block, :, pl.ds(pl.multiple_of(place * cols, 128), cols)]

    def over_sp(d):
        to = lax.rem(me + d, count)
        return pltpu.make_async_remote_copy(
            src_ref=sent_ref.at[:, to], dst_ref=at(me, t), send_sem=sp_send.at[d],
            recv_sem=sp_recv.at[d], device_id={"sp": to}, device_id_type=MESH,
        )

    def over_far(d):
        block = lax.rem(me - d + count, count)
        return pltpu.make_async_remote_copy(
            src_ref=at(block, t), dst_ref=at(block, t), send_sem=far_send.at[d],
            recv_sem=far_recv.at[d], device_id={"tp": far}, device_id_type=MESH,
        )

    def over_near(d, k):
        block = lax.rem(me - d + count, count)
        place = far if k else t
        return pltpu.make_async_remote_copy(
            src_ref=at(block, place), dst_ref=at(block, place), send_sem=near_send.at[k, d],
            recv_sem=near_recv.at[k, d], device_id={"tp": near}, device_id_type=MESH,
        )

    own = pltpu.make_async_copy(sent_ref.at[:, me], at(me, t), own_sem)
    own.start()
    greet(count, me, (far, near))

    def each(body, start=0):
        def step(d, _):
            body(d)
            return 0

        lax.fori_loop(start, count, step, 0)

    each(lambda d: over_sp(d).start(), 1)
    own.wait()
    over_far(0).start()
    over_near(0, 0).start()

    def arrived(d):
        over_sp(d).wait_recv()
        over_far(d).start()
        over_near(d, 0).start()

    each(arrived, 1)

    def crossed(d):
        over_far(d).wait_recv()
        over_near(d, 1).start()

    each(crossed)

    def close(d):
        over_far(d).wait_send()
        over_near(d, 0).wait()
        over_near(d, 1).wait()

    each(close)
    each(lambda d: over_sp(d).wait_send(), 1)


def route(sent, tp):
    two, count, capacity, cols = sent.shape
    dma = pltpu.SemaphoreType.DMA
    return pl.pallas_call(
        partial(route_kernel, count),
        out_shape=jax.ShapeDtypeStruct((two, count, capacity, tp * cols), BF16),
        in_specs=[pl.BlockSpec(memory_space=pltpu.VMEM)],
        out_specs=pl.BlockSpec(memory_space=pltpu.VMEM),
        scratch_shapes=[
            dma(()), dma((count,)), dma((count,)), dma((count,)), dma((count,)),
            dma((2, count)), dma((2, count)),
        ],
        cost_estimate=pl.CostEstimate(
            flops=10_000_000_000, bytes_accessed=8_000_000, transcendentals=0
        ),
        compiler_params=pltpu.CompilerParams(
            collective_id=0, has_side_effects=True, vmem_limit_bytes=32 * 1024 * 1024
        ),
    )(sent)


def fold_kernel(
    count, terms_ref, out_ref, close_ref, pair_ref, away_ref, full_ref,
    own_sem, near_send, near_recv, far_send, far_recv, sp_send, sp_recv,
):
    cols = out_ref.shape[2]
    me = lax.axis_index("sp")
    t, far, near = partners()
    far_near = near + far - t

    def mine(ref, block, place):
        return ref.at[block, :, pl.ds(pl.multiple_of(place * cols, 128), cols)]

    def block_at(d):
        return lax.rem(me + d, count)

    def over_near(d, k):
        return pltpu.make_async_remote_copy(
            src_ref=mine(terms_ref, block_at(d), far_near if k else near),
            dst_ref=close_ref.at[k, d], send_sem=near_send.at[k, d],
            recv_sem=near_recv.at[k, d], device_id={"tp": near}, device_id_type=MESH,
        )

    def over_far(d):
        return pltpu.make_async_remote_copy(
            src_ref=pair_ref.at[d], dst_ref=away_ref.at[d], send_sem=far_send.at[d],
            recv_sem=far_recv.at[d], device_id={"tp": far}, device_id_type=MESH,
        )

    def over_sp(d):
        return pltpu.make_async_remote_copy(
            src_ref=full_ref.at[d], dst_ref=out_ref.at[me], send_sem=sp_send.at[d],
            recv_sem=sp_recv.at[d], device_id={"sp": block_at(d)}, device_id_type=MESH,
        )

    def each(body, start=0):
        def step(d, _):
            body(d)
            return 0

        lax.fori_loop(start, count, step, 0)

    greet(count, me, (far, near))
    order = lambda d: lax.rem(d + 1, count)

    def begin(d):
        over_near(order(d), 1).start()
        over_near(order(d), 0).start()

    each(begin)

    def pair(i):
        d = order(i)
        over_near(d, 1).wait_recv()
        here = mine(terms_ref, block_at(d), far)[...].astype(F32)
        pair_ref[d] = (here + close_ref[1, d].astype(F32)).astype(BF16)
        over_far(d).start()

    each(pair)

    def total(d):
        over_near(d, 0).wait_recv()
        over_far(d).wait_recv()
        here = mine(terms_ref, block_at(d), t)[...].astype(F32)
        here = here + close_ref[0, d].astype(F32) + away_ref[d].astype(F32)
        full_ref[d] = here.astype(BF16)

    def send(d):
        total(d)
        over_sp(d).start()

    each(send, 1)
    total(0)
    own = pltpu.make_async_copy(full_ref.at[0], out_ref.at[me], own_sem)
    own.start()

    def close(d):
        over_near(d, 0).wait_send()
        over_near(d, 1).wait_send()
        over_far(d).wait_send()

    each(close)
    own.wait()
    each(lambda d: over_sp(d).wait(), 1)


def fold(terms, tp):
    count, capacity, width = terms.shape
    cols = width // tp
    dma = pltpu.SemaphoreType.DMA
    part = (count, capacity, cols)
    return pl.pallas_call(
        partial(fold_kernel, count),
        out_shape=jax.ShapeDtypeStruct(part, BF16),
        in_specs=[pl.BlockSpec(memory_space=pltpu.VMEM)],
        out_specs=pl.BlockSpec(memory_space=pltpu.VMEM),
        scratch_shapes=[
            pltpu.VMEM((2,) + part, BF16), pltpu.VMEM(part, BF16), pltpu.VMEM(part, BF16),
            pltpu.VMEM(part, BF16), dma(()), dma((2, count)), dma((2, count)), dma((count,)),
            dma((count,)), dma((count,)), dma((count,)),
        ],
        cost_estimate=pl.CostEstimate(
            flops=10_000_000_000, bytes_accessed=4_000_000, transcendentals=0
        ),
        compiler_params=pltpu.CompilerParams(
            collective_id=1, has_side_effects=True, vmem_limit_bytes=32 * 1024 * 1024
        ),
    )(terms)


def carries(last, axis):
    count, me = lax.axis_size(axis), lax.axis_index(axis)
    ends = lax.all_gather(last, axis)
    j = jnp.arange(count)
    i = j[None, :]
    ahead = ((i > j[:, None]) & (i < me)).astype(F32)
    behind = ((i < j[:, None]) & (i > me)).astype(F32)
    fore = jnp.where((j < me)[:, None], jnp.exp(jnp.dot(ahead, ends, precision=HIGH)), 0.0)
    back = jnp.where((j > me)[:, None], jnp.exp(jnp.dot(behind, ends, precision=HIGH)), 0.0)
    return fore, back


def body(
    moe_input, cotangent, expert_ids, routing_weights, gate_weight, up_weight, down_weight,
    inner_x, inner_b, inner_c, gate_z, step_raw, decay_rate, skip_weight, norm_gain, w_out,
):
    rows, chosen = expert_ids.shape
    senders = lax.axis_size("sp")
    experts = gate_weight.shape[0] * senders
    capacity = 4 * rows // experts
    slots = experts * capacity
    cols = moe_input.shape[1]
    heads = decay_rate.shape[0]
    inner = heads * HEAD_DIM
    rate, skip, gain = decay_rate[None, :], skip_weight[None, :], norm_gain[None, :]

    dt = jax.nn.softplus(step_raw)
    run = jnp.cumsum(-dt * rate, axis=0)
    run_t = run.T
    (fresh,) = call(fresh_kernel, [((STATE, inner), BF16)], 40_000_000)(inner_x, inner_b, dt, run)
    fresh_all = lax.all_gather(fresh, "sp")
    fore, back = carries(run[-1], "sp")

    (sent,) = call(partial(dispatch_kernel, experts), [((2, slots, cols), BF16)], 200_000_000)(
        moe_input, cotangent, expert_ids, routing_weights
    )
    tp = lax.axis_size("tp")
    routed = route(sent.reshape(2, senders, slots // senders, cols), tp)
    routed = routed.reshape(2, slots, tp * cols)
    routed_in, routed_grad = routed[0], routed[1]

    weight_rows = pltpu.VMEM((senders, inner), F32)
    norm_rows, mixed, state = call(
        forward_kernel,
        [((rows, inner), BF16), ((rows, inner), F32), ((STATE, inner), F32)],
        300_000_000,
        [weight_rows],
    )(inner_x, inner_b, inner_c, gate_z, dt, run, run_t, skip, gain, fresh_all, fore)
    norm_all = lax.all_gather(norm_rows, "sp", axis=0, tiled=True)

    gate_w, up_w, down_w = gate_weight[0], up_weight[0], down_weight[0]
    gate_pre = jnp.dot(routed_in, gate_w, preferred_element_type=F32)
    up_pre = jnp.dot(routed_in, up_w, preferred_element_type=F32)
    sig = jax.nn.sigmoid(gate_pre)
    active = gate_pre * sig
    hidden = (active * up_pre).astype(BF16)
    hidden_grad = nt(routed_grad, down_w)
    gate_grad = (hidden_grad * up_pre * sig * (1.0 + gate_pre * (1.0 - sig))).astype(BF16)
    up_grad = (hidden_grad * active).astype(BF16)
    terms = (nt(gate_grad, gate_w) + nt(up_grad, up_w)).astype(BF16)
    returned = fold(terms.reshape(senders, slots // senders, tp * cols), tp).reshape(slots, cols)
    (mixer_cols,) = call(partial(combine_kernel, experts), [((rows, cols), BF16)], 100_000_000)(
        returned, cotangent, expert_ids
    )
    mixer_rows = lax.all_gather(mixer_cols, "tp", axis=1, tiled=True)
    norm_grad = jnp.dot(mixer_rows, w_out, preferred_element_type=F32)
    state_grad, xs_grad, x_grad, z_grad, run_grad, b_grad, c_grad = call(
        backward_kernel,
        [
            ((STATE, inner), BF16),
            ((rows, inner), F32),
            ((rows, inner), F32),
            ((rows, inner), BF16),
            ((rows, heads), F32),
            ((rows, STATE), F32),
            ((rows, STATE), F32),
        ],
        600_000_000,
    )(inner_x, inner_b, inner_c, gate_z, dt, run, run_t, skip, gain, mixed, state, norm_grad)
    state_grads = lax.all_gather(state_grad, "sp")
    depth = mixer_rows.shape[1] // senders
    mixer_blocks = jnp.swapaxes(mixer_rows.reshape(rows, senders, depth), 0, 1)
    mixer_all = lax.all_to_all(mixer_blocks, "sp", 0, 0, tiled=True).reshape(rows * senders, depth)
    grad_out = tn(mixer_all, norm_all)
    gate_weight_gradient = tn(routed_in, gate_grad).astype(BF16)[None]
    up_weight_gradient = tn(routed_in, up_grad).astype(BF16)[None]
    down_weight_gradient = tn(hidden, routed_grad).astype(BF16)[None]
    grad_inner_x, grad_inner_b, grad_step_raw = call(
        finish_kernel,
        [((rows, inner), BF16), ((rows, STATE), F32), ((rows, heads), F32)],
        300_000_000,
        [weight_rows],
    )(
        inner_x, inner_b, step_raw, dt, run, rate, state, state_grads, back, xs_grad, x_grad,
        run_grad, b_grad,
    )
    return (
        gate_weight_gradient, up_weight_gradient, down_weight_gradient, grad_out, grad_inner_x,
        grad_inner_b, c_grad, z_grad, grad_step_raw,
    )


def solution(mesh):
    row = P("sp", "tp")
    deep, flat, tall = P("sp", None, "tp"), P("sp", None), P("sp", "tp", None)
    return jax.shard_map(
        body,
        mesh=mesh,
        in_specs=(
            row, row, flat, flat, deep, deep, tall, row, row, row, row, row,
            P("tp"), P("tp"), P("tp"), P(None, "tp"),
        ),
        out_specs=(deep, deep, tall, row, row, row, row, row, row),
        check_vma=False,
    )
```

```python
from functools import partial

import jax
import jax.numpy as jnp
from jax import lax
from jax.experimental import pallas as pl
from jax.experimental.pallas import tpu as pltpu
from jax.sharding import PartitionSpec as P

HEAD_DIM = 64
STATE = 64
PAIR = 2 * HEAD_DIM
EPS = 0.01
EXTRA = 16
HIGH = lax.Precision.HIGHEST
F32 = jnp.float32
BF16 = jnp.bfloat16


def call(kernel, outs, flops, scratch=()):
    return pl.pallas_call(
        kernel,
        out_shape=[jax.ShapeDtypeStruct(s, d) for s, d in outs],
        scratch_shapes=list(scratch),
        cost_estimate=pl.CostEstimate(flops=flops, bytes_accessed=4_000_000, transcendentals=0),
        compiler_params=pltpu.CompilerParams(vmem_limit_bytes=48 * 1024 * 1024),
    )


def nn(a, b):
    return jnp.dot(a.astype(BF16), b.astype(BF16), preferred_element_type=F32)


def tn(a, b):
    return lax.dot_general(
        a.astype(BF16), b.astype(BF16), (((0,), (0,)), ((), ())), preferred_element_type=F32
    )


def nt(a, b):
    return lax.dot_general(
        a.astype(BF16), b.astype(BF16), (((1,), (1,)), ((), ())), preferred_element_type=F32
    )


def spread(heads):
    rows = lax.broadcasted_iota(jnp.int32, (heads, heads * HEAD_DIM), 0)
    cols = lax.broadcasted_iota(jnp.int32, (heads, heads * HEAD_DIM), 1)
    return (cols // HEAD_DIM == rows).astype(F32)


def wide(v, table):
    return jnp.dot(v, table, precision=HIGH, preferred_element_type=F32)


def narrow(v, table):
    return lax.dot_general(
        v, table, (((1,), (1,)), ((), ())), precision=HIGH, preferred_element_type=F32
    )


def silu_and_slope(v):
    s = jax.nn.sigmoid(v)
    return v * s, s * (1.0 + v * (1.0 - s))


def silu(v):
    return v * jax.nn.sigmoid(v)


def causal_of(rows):
    return lax.broadcasted_iota(jnp.int32, (rows, rows), 0) >= lax.broadcasted_iota(
        jnp.int32, (rows, rows), 1
    )


def decay_table(causal, run_ref, run_t_ref, head):
    gap = run_ref[:, head : head + 1] - run_t_ref[head : head + 1, :]
    return jnp.where(causal, jnp.exp(jnp.where(causal, gap, 0.0)), 0.0)


def fresh_kernel(x_ref, b_ref, dt_ref, run_ref, fresh_ref):
    table = spread(dt_ref.shape[1])
    run = run_ref[...]
    factor = dt_ref[...] * jnp.exp(run[-1:, :] - run)
    xe = silu(x_ref[...].astype(F32)) * wide(factor, table)
    fresh_ref[:STATE, :] = tn(silu(b_ref[...].astype(F32)), xe).astype(BF16)
    rest = wide(jnp.broadcast_to(run[-1:, :], (EXTRA, run.shape[1])), table)
    row = lax.broadcasted_iota(jnp.int32, rest.shape, 0)
    extra = jnp.zeros_like(rest)
    for k in range(3):
        piece = rest.astype(BF16).astype(F32)
        extra = jnp.where(row == k, piece, extra)
        rest = rest - piece
    fresh_ref[STATE:, :] = extra.astype(BF16)


def weighted_sum(all_ref, weight_ref):
    def one(j, total):
        return total + all_ref[j, :STATE, :].astype(F32) * weight_ref[pl.ds(j, 1), :]

    return lax.fori_loop(0, all_ref.shape[0], one, jnp.zeros((STATE, all_ref.shape[2]), F32))


def fill_carries(all_ref, ends_ref, fore_ref, back_ref):
    count = all_ref.shape[0]
    me = lax.axis_index("sp")

    def one(j, _):
        parts = all_ref[j, STATE:, :].astype(F32)
        ends_ref[pl.ds(j, 1), :] = parts[0:1] + parts[1:2] + parts[2:3]
        return 0

    lax.fori_loop(0, count, one, 0)
    j = lax.broadcasted_iota(jnp.int32, (count, count), 0)
    i = lax.broadcasted_iota(jnp.int32, (count, count), 1)
    own = lax.broadcasted_iota(jnp.int32, fore_ref.shape, 0)
    ahead = ((i > j) & (i < me)).astype(F32)
    behind = ((i < j) & (i > me)).astype(F32)
    fore_ref[...] = jnp.where(own < me, jnp.exp(wide(ahead, ends_ref[...])), 0.0)
    back_ref[...] = jnp.where(own > me, jnp.exp(wide(behind, ends_ref[...])), 0.0)


def forward_kernel(
    x_ref, b_ref, c_ref, z_ref, dt_ref, run_ref, run_t_ref, skip_ref, gain_ref, all_ref,
    norm_ref, mixed_ref, state_ref, back_ref, weight_ref, ends_ref,
):
    heads = dt_ref.shape[1]
    table = spread(heads)
    fill_carries(all_ref, ends_ref, weight_ref, back_ref)
    state = weighted_sum(all_ref, weight_ref)
    state_ref[...] = state
    x_act = silu(x_ref[...].astype(F32))
    xs = (x_act * wide(dt_ref[...], table)).astype(BF16)
    b_act = silu(b_ref[...].astype(F32))
    c_act = silu(c_ref[...].astype(F32))
    mixed_ref[...] = nn(c_act, state) * wide(jnp.exp(run_ref[...]), table) + x_act * wide(
        skip_ref[...], table
    )
    rows = x_ref.shape[0]
    causal = causal_of(rows)
    scores = nt(c_act, b_act)
    first = lax.broadcasted_iota(jnp.int32, (rows, PAIR), 1) < HEAD_DIM
    for pair in range(heads // 2):
        lo = pair * PAIR
        part = xs[:, lo : lo + PAIR]
        one = nn(scores * decay_table(causal, run_ref, run_t_ref, 2 * pair), part)
        two = nn(scores * decay_table(causal, run_ref, run_t_ref, 2 * pair + 1), part)
        mixed_ref[:, lo : lo + PAIR] += jnp.where(first, one, two)
    gated = mixed_ref[...] * silu(z_ref[...].astype(F32))
    scale = lax.rsqrt(jnp.mean(gated * gated, axis=1, keepdims=True) + EPS)
    norm_ref[...] = (gated * scale * gain_ref[...]).astype(BF16)


def backward_kernel(
    x_ref, b_ref, c_ref, z_ref, dt_ref, run_ref, run_t_ref, skip_ref, gain_ref, mixed_ref,
    state_ref, up_ref,
    state_grad_ref, xs_grad_ref, x_grad_ref, z_grad_ref, run_grad_ref, b_grad_ref, c_grad_ref,
):
    heads = dt_ref.shape[1]
    rows = x_ref.shape[0]
    table = spread(heads)
    z_act, z_slope = silu_and_slope(z_ref[...].astype(F32))
    mixed = mixed_ref[...]
    gated = mixed * z_act
    scale = lax.rsqrt(jnp.mean(gated * gated, axis=1, keepdims=True) + EPS)
    up = up_ref[...] * gain_ref[...]
    inner = jnp.mean(up * gated, axis=1, keepdims=True)
    gated_grad = scale * (up - gated * (scale * scale * inner))
    z_grad_ref[...] = (gated_grad * mixed * z_slope).astype(BF16)
    dy = gated_grad * z_act
    x_act = silu(x_ref[...].astype(F32))
    x_grad_ref[...] = dy * wide(skip_ref[...], table)
    xs = (x_act * wide(dt_ref[...], table)).astype(BF16)
    b_act = silu(b_ref[...].astype(F32))
    c_act, c_slope = silu_and_slope(c_ref[...].astype(F32))
    state = state_ref[...]
    grown = dy * wide(jnp.exp(run_ref[...]), table)
    state_grad_ref[...] = tn(c_act, grown).astype(BF16)
    c_grad = nt(grown, state)
    run_grad = narrow(grown * nn(c_act, state), table)
    causal = causal_of(rows)
    scores = nt(c_act, b_act)
    scores_grad = jnp.zeros((rows, rows), F32)
    first = lax.broadcasted_iota(jnp.int32, (rows, PAIR), 1) < HEAD_DIM
    lane = lax.broadcasted_iota(jnp.int32, (rows, heads), 1)
    for pair in range(heads // 2):
        lo = pair * PAIR
        part = xs[:, lo : lo + PAIR]
        dy_part = dy[:, lo : lo + PAIR]
        got = []
        for k in range(2):
            head = 2 * pair + k
            decay = decay_table(causal, run_ref, run_t_ref, head)
            weights = scores * decay
            mine = jnp.where(first if k == 0 else ~first, dy_part, 0.0)
            got.append(tn(weights, mine))
            weights_grad = nt(mine, part)
            scores_grad += weights_grad * decay
            flow = weights_grad * weights
            change = jnp.sum(flow - flow.T, axis=1, keepdims=True)
            run_grad += jnp.where(lane == head, change, 0.0)
        xs_grad_ref[:, lo : lo + PAIR] = got[0] + got[1]
    run_grad_ref[...] = run_grad
    b_grad_ref[...] = tn(scores_grad, c_act)
    c_grad_ref[...] = (c_grad + nn(scores_grad, b_act)) * c_slope


def finish_kernel(
    x_ref, b_ref, raw_ref, dt_ref, run_ref, rate_ref, state_ref, all_ref, coef_ref, xs_grad_ref,
    x_grad_ref, run_grad_ref, b_grad_ref,
    x_out_ref, b_out_ref, raw_out_ref,
):
    heads = dt_ref.shape[1]
    rows = x_ref.shape[0]
    table = spread(heads)
    after = weighted_sum(all_ref, coef_ref)
    x_act, x_slope = silu_and_slope(x_ref[...].astype(F32))
    b_act, b_slope = silu_and_slope(b_ref[...].astype(F32))
    dt = dt_ref[...]
    dt_wide = wide(dt, table)
    run = run_ref[...]
    last = run[-1:, :]
    to_end = wide(jnp.exp(last - run), table)
    moved = nn(b_act, after) * to_end
    xs = x_act * dt_wide
    xs_grad = xs_grad_ref[...] + moved
    b_grad = b_grad_ref[...] + nt(xs * to_end, after)
    out_flow = narrow(xs * moved, table)
    whole = jnp.exp(last) * narrow(
        jnp.sum(after * state_ref[...], axis=0, keepdims=True), table
    )
    at_end = jnp.sum(out_flow, axis=0, keepdims=True) + whole
    run_grad = run_grad_ref[...] - out_flow
    causal = causal_of(rows).astype(F32)
    log_grad = at_end + lax.dot_general(
        causal, run_grad, (((0,), (0,)), ((), ())), precision=HIGH, preferred_element_type=F32
    )
    dt_grad = narrow(x_act * xs_grad, table) - rate_ref[...] * log_grad
    raw_out_ref[...] = dt_grad * jax.nn.sigmoid(raw_ref[...])
    b_out_ref[...] = b_grad * b_slope
    x_out_ref[...] = ((x_grad_ref[...] + xs_grad * dt_wide) * x_slope).astype(BF16)


def picks(ids, slots, experts):
    rows = ids.shape[0]
    capacity = slots // experts
    choice = lax.broadcasted_iota(jnp.int32, (rows, experts), 1)
    hot = [(ids[:, k : k + 1] == choice).astype(F32) for k in range(ids.shape[1])]
    strict = (
        lax.broadcasted_iota(jnp.int32, (rows, rows), 0)
        > lax.broadcasted_iota(jnp.int32, (rows, rows), 1)
    ).astype(F32)
    before = nn(strict, sum(hot))
    place = lax.broadcasted_iota(jnp.int32, (rows, slots), 1)
    found = []
    for k, one in enumerate(hot):
        rank = jnp.sum(before * one, axis=1, keepdims=True).astype(jnp.int32)
        found.append((place == ids[:, k : k + 1] * capacity + rank).astype(BF16))
    return found


def dispatch_kernel(experts, x_ref, cot_ref, ids_ref, weight_ref, out_ref):
    slots = out_ref.shape[1]
    cols = x_ref.shape[1]
    found = picks(ids_ref[...], slots, experts)
    cot = cot_ref[...].astype(F32)
    total = jnp.zeros((slots, cols), F32)
    for k, one in enumerate(found):
        total += tn(one, (cot * weight_ref[:, k : k + 1]).astype(BF16))
    out_ref[0] = tn(sum(found), x_ref[...]).astype(BF16)
    out_ref[1] = total.astype(BF16)


def combine_kernel(experts, back_ref, cot_ref, ids_ref, out_ref):
    found = picks(ids_ref[...], back_ref.shape[0], experts)
    moe_grad = nn(sum(found), back_ref[...])
    out_ref[...] = (cot_ref[...].astype(F32) + moe_grad).astype(BF16)


MESH = pl.DeviceIdType.MESH


def greet(count, me, others):
    barrier = pltpu.get_barrier_semaphore()

    def one(d, _):
        pl.semaphore_signal(
            barrier, inc=1, device_id={"sp": lax.rem(me + d, count)}, device_id_type=MESH
        )
        return 0

    lax.fori_loop(1, count, one, 0)
    for other in others:
        pl.semaphore_signal(barrier, inc=1, device_id={"tp": other}, device_id_type=MESH)
    pl.semaphore_wait(barrier, count - 1 + len(others))


def partners():
    t = lax.axis_index("tp")
    half = lax.axis_size("tp") // 2
    far = lax.rem(t + half, 2 * half)
    near = t + 1 - 2 * lax.rem(t, 2)
    return t, far, near


def route_kernel(
    count, sent_ref, out_ref, own_sem, sp_send, sp_recv, far_send, far_recv, near_send, near_recv
):
    cols = sent_ref.shape[3]
    me = lax.axis_index("sp")
    t, far, near = partners()

    def at(block, place):
        return out_ref.at[:, block, :, pl.ds(pl.multiple_of(place * cols, 128), cols)]

    def over_sp(d):
        to = lax.rem(me + d, count)
        return pltpu.make_async_remote_copy(
            src_ref=sent_ref.at[:, to], dst_ref=at(me, t), send_sem=sp_send.at[d],
            recv_sem=sp_recv.at[d], device_id={"sp": to}, device_id_type=MESH,
        )

    def over_far(d):
        block = lax.rem(me - d + count, count)
        return pltpu.make_async_remote_copy(
            src_ref=at(block, t), dst_ref=at(block, t), send_sem=far_send.at[d],
            recv_sem=far_recv.at[d], device_id={"tp": far}, device_id_type=MESH,
        )

    def over_near(d, k):
        block = lax.rem(me - d + count, count)
        place = far if k else t
        return pltpu.make_async_remote_copy(
            src_ref=at(block, place), dst_ref=at(block, place), send_sem=near_send.at[k, d],
            recv_sem=near_recv.at[k, d], device_id={"tp": near}, device_id_type=MESH,
        )

    own = pltpu.make_async_copy(sent_ref.at[:, me], at(me, t), own_sem)
    own.start()
    greet(count, me, (far, near))

    def each(body, start=0):
        def step(d, _):
            body(d)
            return 0

        lax.fori_loop(start, count, step, 0)

    each(lambda d: over_sp(d).start(), 1)
    own.wait()
    over_far(0).start()
    over_near(0, 0).start()

    def arrived(d):
        over_sp(d).wait_recv()
        over_far(d).start()
        over_near(d, 0).start()

    each(arrived, 1)

    def crossed(d):
        over_far(d).wait_recv()
        over_near(d, 1).start()

    each(crossed)

    def close(d):
        over_far(d).wait_send()
        over_near(d, 0).wait()
        over_near(d, 1).wait()

    each(close)
    each(lambda d: over_sp(d).wait_send(), 1)


def route(sent, tp):
    two, count, capacity, cols = sent.shape
    dma = pltpu.SemaphoreType.DMA
    return pl.pallas_call(
        partial(route_kernel, count),
        out_shape=jax.ShapeDtypeStruct((two, count, capacity, tp * cols), BF16),
        in_specs=[pl.BlockSpec(memory_space=pltpu.VMEM)],
        out_specs=pl.BlockSpec(memory_space=pltpu.VMEM),
        scratch_shapes=[
            dma(()), dma((count,)), dma((count,)), dma((count,)), dma((count,)),
            dma((2, count)), dma((2, count)),
        ],
        cost_estimate=pl.CostEstimate(
            flops=10_000_000_000, bytes_accessed=8_000_000, transcendentals=0
        ),
        compiler_params=pltpu.CompilerParams(
            collective_id=0, has_side_effects=True, vmem_limit_bytes=32 * 1024 * 1024
        ),
    )(sent)


def fold_kernel(
    count, terms_ref, out_ref, close_ref, pair_ref, away_ref, full_ref,
    own_sem, near_send, near_recv, far_send, far_recv, sp_send, sp_recv,
):
    cols = out_ref.shape[2]
    me = lax.axis_index("sp")
    t, far, near = partners()
    far_near = near + far - t

    def mine(ref, block, place):
        return ref.at[block, :, pl.ds(pl.multiple_of(place * cols, 128), cols)]

    def block_at(d):
        return lax.rem(me + d, count)

    def over_near(d, k):
        return pltpu.make_async_remote_copy(
            src_ref=mine(terms_ref, block_at(d), far_near if k else near),
            dst_ref=close_ref.at[k, d], send_sem=near_send.at[k, d],
            recv_sem=near_recv.at[k, d], device_id={"tp": near}, device_id_type=MESH,
        )

    def over_far(d):
        return pltpu.make_async_remote_copy(
            src_ref=pair_ref.at[d], dst_ref=away_ref.at[d], send_sem=far_send.at[d],
            recv_sem=far_recv.at[d], device_id={"tp": far}, device_id_type=MESH,
        )

    def over_sp(d):
        return pltpu.make_async_remote_copy(
            src_ref=full_ref.at[d], dst_ref=out_ref.at[me], send_sem=sp_send.at[d],
            recv_sem=sp_recv.at[d], device_id={"sp": block_at(d)}, device_id_type=MESH,
        )

    def each(body, start=0):
        def step(d, _):
            body(d)
            return 0

        lax.fori_loop(start, count, step, 0)

    greet(count, me, (far, near))
    order = lambda d: lax.rem(d + 1, count)

    def begin(d):
        over_near(order(d), 1).start()
        over_near(order(d), 0).start()

    each(begin)

    def pair(i):
        d = order(i)
        over_near(d, 1).wait_recv()
        here = mine(terms_ref, block_at(d), far)[...].astype(F32)
        pair_ref[d] = (here + close_ref[1, d].astype(F32)).astype(BF16)
        over_far(d).start()

    each(pair)

    def total(d):
        over_near(d, 0).wait_recv()
        over_far(d).wait_recv()
        here = mine(terms_ref, block_at(d), t)[...].astype(F32)
        here = here + close_ref[0, d].astype(F32) + away_ref[d].astype(F32)
        full_ref[d] = here.astype(BF16)

    def send(d):
        total(d)
        over_sp(d).start()

    each(send, 1)
    total(0)
    own = pltpu.make_async_copy(full_ref.at[0], out_ref.at[me], own_sem)
    own.start()

    def close(d):
        over_near(d, 0).wait_send()
        over_near(d, 1).wait_send()
        over_far(d).wait_send()

    each(close)
    own.wait()
    each(lambda d: over_sp(d).wait(), 1)


def fold(terms, tp):
    count, capacity, width = terms.shape
    cols = width // tp
    dma = pltpu.SemaphoreType.DMA
    part = (count, capacity, cols)
    return pl.pallas_call(
        partial(fold_kernel, count),
        out_shape=jax.ShapeDtypeStruct(part, BF16),
        in_specs=[pl.BlockSpec(memory_space=pltpu.VMEM)],
        out_specs=pl.BlockSpec(memory_space=pltpu.VMEM),
        scratch_shapes=[
            pltpu.VMEM((2,) + part, BF16), pltpu.VMEM(part, BF16), pltpu.VMEM(part, BF16),
            pltpu.VMEM(part, BF16), dma(()), dma((2, count)), dma((2, count)), dma((count,)),
            dma((count,)), dma((count,)), dma((count,)),
        ],
        cost_estimate=pl.CostEstimate(
            flops=10_000_000_000, bytes_accessed=4_000_000, transcendentals=0
        ),
        compiler_params=pltpu.CompilerParams(
            collective_id=1, has_side_effects=True, vmem_limit_bytes=32 * 1024 * 1024
        ),
    )(terms)


def body(
    moe_input, cotangent, expert_ids, routing_weights, gate_weight, up_weight, down_weight,
    inner_x, inner_b, inner_c, gate_z, step_raw, decay_rate, skip_weight, norm_gain, w_out,
):
    rows, chosen = expert_ids.shape
    senders = lax.axis_size("sp")
    experts = gate_weight.shape[0] * senders
    capacity = 4 * rows // experts
    slots = experts * capacity
    cols = moe_input.shape[1]
    heads = decay_rate.shape[0]
    inner = heads * HEAD_DIM
    rate, skip, gain = decay_rate[None, :], skip_weight[None, :], norm_gain[None, :]

    dt = jax.nn.softplus(step_raw)
    run = jnp.cumsum(-dt * rate, axis=0)
    run_t = run.T
    (fresh,) = call(fresh_kernel, [((STATE + EXTRA, inner), BF16)], 40_000_000)(inner_x, inner_b, dt, run)
    fresh_all = lax.all_gather(fresh, "sp")

    (sent,) = call(partial(dispatch_kernel, experts), [((2, slots, cols), BF16)], 200_000_000)(
        moe_input, cotangent, expert_ids, routing_weights
    )
    tp = lax.axis_size("tp")
    routed = route(sent.reshape(2, senders, slots // senders, cols), tp)
    routed = routed.reshape(2, slots, tp * cols)
    routed_in, routed_grad = routed[0], routed[1]

    weight_rows = pltpu.VMEM((senders, inner), F32)
    norm_rows, mixed, state, back = call(
        forward_kernel,
        [((rows, inner), BF16), ((rows, inner), F32), ((STATE, inner), F32), ((senders, inner), F32)],
        300_000_000,
        [weight_rows, weight_rows],
    )(inner_x, inner_b, inner_c, gate_z, dt, run, run_t, skip, gain, fresh_all)

    gate_w, up_w, down_w = gate_weight[0], up_weight[0], down_weight[0]
    gate_pre = jnp.dot(routed_in, gate_w, preferred_element_type=F32)
    up_pre = jnp.dot(routed_in, up_w, preferred_element_type=F32)
    sig = jax.nn.sigmoid(gate_pre)
    active = gate_pre * sig
    hidden = (active * up_pre).astype(BF16)
    hidden_grad = nt(routed_grad, down_w)
    gate_grad = (hidden_grad * up_pre * sig * (1.0 + gate_pre * (1.0 - sig))).astype(BF16)
    up_grad = (hidden_grad * active).astype(BF16)
    terms = (nt(gate_grad, gate_w) + nt(up_grad, up_w)).astype(BF16)
    terms, norm_rows = lax.optimization_barrier((terms, norm_rows))
    norm_all = lax.all_gather(norm_rows, "sp", axis=0, tiled=True)
    returned = fold(terms.reshape(senders, slots // senders, tp * cols), tp).reshape(slots, cols)
    (mixer_cols,) = call(partial(combine_kernel, experts), [((rows, cols), BF16)], 100_000_000)(
        returned, cotangent, expert_ids
    )
    mixer_rows = lax.all_gather(mixer_cols, "tp", axis=1, tiled=True)
    norm_grad = jnp.dot(mixer_rows, w_out, preferred_element_type=F32)
    norm_grad, norm_all = lax.optimization_barrier((norm_grad, norm_all))
    state_grad, xs_grad, x_grad, z_grad, run_grad, b_grad, c_grad = call(
        backward_kernel,
        [
            ((STATE, inner), BF16),
            ((rows, inner), F32),
            ((rows, inner), F32),
            ((rows, inner), BF16),
            ((rows, heads), F32),
            ((rows, STATE), F32),
            ((rows, STATE), F32),
        ],
        600_000_000,
    )(inner_x, inner_b, inner_c, gate_z, dt, run, run_t, skip, gain, mixed, state, norm_grad)
    state_grads = lax.all_gather(state_grad, "sp")
    depth = mixer_rows.shape[1] // senders
    mixer_blocks = jnp.swapaxes(mixer_rows.reshape(rows, senders, depth), 0, 1)
    mixer_all = lax.all_to_all(mixer_blocks, "sp", 0, 0, tiled=True).reshape(rows * senders, depth)
    grad_out = tn(mixer_all, norm_all)
    gate_weight_gradient = tn(routed_in, gate_grad).astype(BF16)[None]
    up_weight_gradient = tn(routed_in, up_grad).astype(BF16)[None]
    down_weight_gradient = tn(hidden, routed_grad).astype(BF16)[None]
    grad_inner_x, grad_inner_b, grad_step_raw = call(
        finish_kernel,
        [((rows, inner), BF16), ((rows, STATE), F32), ((rows, heads), F32)],
        300_000_000,
    )(
        inner_x, inner_b, step_raw, dt, run, rate, state, state_grads, back, xs_grad, x_grad,
        run_grad, b_grad,
    )
    return (
        gate_weight_gradient, up_weight_gradient, down_weight_gradient, grad_out, grad_inner_x,
        grad_inner_b, c_grad, z_grad, grad_step_raw,
    )


def solution(mesh):
    row = P("sp", "tp")
    deep, flat, tall = P("sp", None, "tp"), P("sp", None), P("sp", "tp", None)
    return jax.shard_map(
        body,
        mesh=mesh,
        in_specs=(
            row, row, flat, flat, deep, deep, tall, row, row, row, row, row,
            P("tp"), P("tp"), P("tp"), P(None, "tp"),
        ),
        out_specs=(deep, deep, tall, row, row, row, row, row, row),
        check_vma=False,
    )
```
